32 devices in a mesh: sp: 16 (over z, y, x), tp: 2 (over core).
Axes of the slice: x: 2, y: 2, z: 4, core: 2. Of those that a mesh axis runs over, the one named last changes fastest.
Arguments:
- tokens: bfloat16 [6144, 2048], P('sp', 'tp'), may hold values from -40 to 40
- mix_gain: float32 [2048], replicated, may hold values from 0.1 to 1.9
- w_pool_in: bfloat16 [2048, 1024], P(None, 'tp'), may hold values from -0.125 to 0.125
- w_qlat: bfloat16 [2048, 512], P(None, 'tp'), may hold values from -0.125 to 0.125
- w_kvlat: bfloat16 [2048, 512], P(None, 'tp'), may hold values from -0.125 to 0.125
- w_krope: bfloat16 [2048, 64], replicated, may hold values from -0.125 to 0.125
- q_gain: float32 [512], replicated, may hold values from 1 to 60
- kv_gain: float32 [512], replicated, may hold values from 0.1 to 1.9
- w_q_content: bfloat16 [512, 2048], P(None, 'tp'), may hold values from -0.25 to 0.25
- w_q_rotary: bfloat16 [512, 1024], P(None, 'tp'), may hold values from -0.25 to 0.25
- w_key: bfloat16 [512, 2048], P(None, 'tp'), may hold values from -0.25 to 0.25
- w_value: bfloat16 [512, 2048], P(None, 'tp'), may hold values from -0.25 to 0.25
- pool_mix: bfloat16 [8, 128, 128], replicated, may hold values from -0.5 to 0.5
- pool_scale: float32 [1024], replicated, may hold values from 0.1 to 1.9
- w_out_pool: bfloat16 [1024, 2048], P('tp'), may hold values from -0.109375 to 0.109375
- w_out_attn: bfloat16 [2048, 2048], P('tp'), may hold values from -0.25 to 0.25
Outputs:
- layer_out: bfloat16 [6144, 2048], P(('sp', 'tp'))
- log_total: float32 [6144, 16], P('sp', 'tp')
The draws below stay inside these ranges and needn't reach their ends.
All inputs are finite; a program needn't handle non-finite values.
Results may differ from the reference program's by a relative error of at most 0.015.
The reference program's roundings to bfloat16 on the way (of `scaled`, `weights`, `attended`, `pooled` and `pool_out`) count: a program that leaves them out, or rounds other values in their place, can miss the bound.
Values may be sent and summed in bfloat16 or wider, within the bound.
A program may use at most 64 MiB of HBM per device.

```python
import jax
import jax.numpy as jnp
from jax import lax

D = 2048
HEADS = 16
NOPE = 128
ROPE = 64
VDIM = 128
QLAT = 512
KVLAT = 512
GROUPS = 8
GROUP_DIM = 128
WIDEST = 16
SPAN = 16
TOK_DEV = 384
POOL = 1024
MIX = 3072
SEQ_LEN = 6144
SEQS = 1
TOKENS = 6144


def draw_tokens(key, part):
    base_key, column_key = jax.random.split(jax.random.fold_in(key, 11), 2)
    base = jnp.clip(jax.random.normal(base_key, (TOKENS, D), jnp.float32), -6.0, 6.0)
    ramp = jnp.arange(D, dtype=jnp.float32) / D
    column_scale = jnp.exp(jnp.log(4.0) * ramp + jax.random.uniform(column_key, (D,), jnp.float32, -0.5, 0.5))
    return jnp.clip(base * column_scale[None, :], -40.0, 40.0).astype(jnp.bfloat16)


def draw_q_gain(key, part):
    gain_key = jax.random.fold_in(key, 23)
    logs = jax.random.uniform(gain_key, (QLAT,), jnp.float32, 0.0, jnp.log(4.0))
    return jnp.exp(logs)


def steps_of(own_key, shape, cuts, least, high):
    gain, own = 1.0, jax.random.fold_in(own_key, 6)
    for axis_at, parts in cuts:
        heights = jnp.exp(jax.random.uniform(jax.random.fold_in(own, axis_at), (parts,), jnp.float32, least / len(cuts), high / len(cuts)))
        gain = gain * jnp.repeat(heights, shape[axis_at] // parts).reshape([-1 if axis == axis_at else 1 for axis in range(len(shape))])
    return gain


def normal_values(key, extent, spread, most, shards=(), kind=jnp.bfloat16):
    drawn = jax.random.normal(key, extent, jnp.float32) * spread
    if len(shards) > 0:
        drawn = steps_of(key, extent, shards, -0.22, 0.18) * drawn
    return jnp.clip(drawn, min=-most, max=most).astype(kind)


def setup_inputs(seed: int = 0) -> dict:
    keys = jax.random.split(jax.random.key(seed), 17)
    tokens = draw_tokens(jax.random.fold_in(keys[16], 71), 0)
    mix_gain = jnp.clip(1.0 + 0.18 * jax.random.normal(keys[1], (D,), jnp.float32), 0.1, 1.9)
    w_pool_in = normal_values(keys[2], (D, POOL), D ** -0.5, 0.125, ((1, 2),))
    w_qlat = normal_values(keys[3], (D, QLAT), D ** -0.5, 0.125, ((1, 2),))
    w_kvlat = normal_values(keys[4], (D, KVLAT), D ** -0.5, 0.125, ((1, 2),))
    w_krope = normal_values(keys[5], (D, ROPE), D ** -0.5, 0.125)
    q_gain = draw_q_gain(jax.random.fold_in(keys[16], 71), 0)
    kv_gain = jnp.clip(1.0 + 0.18 * jax.random.normal(keys[7], (KVLAT,), jnp.float32), 0.1, 1.9)
    w_q_content = normal_values(keys[8], (QLAT, HEADS * NOPE), QLAT ** -0.5, 0.25, ((1, 2),))
    w_q_rotary = normal_values(keys[9], (QLAT, HEADS * ROPE), QLAT ** -0.5, 0.25, ((1, 2),))
    w_key = normal_values(keys[10], (KVLAT, HEADS * NOPE), KVLAT ** -0.5, 0.25, ((1, 2),))
    w_value = normal_values(keys[11], (KVLAT, HEADS * VDIM), KVLAT ** -0.5, 0.25, ((1, 2),))
    pool_mix = normal_values(keys[12], (GROUPS, GROUP_DIM, GROUP_DIM), GROUP_DIM ** -0.5, 0.5)
    pool_scale = jnp.clip(1.0 + 0.18 * jax.random.normal(keys[13], (POOL,), jnp.float32), 0.1, 1.9)
    w_out_pool = normal_values(keys[14], (POOL, D), MIX ** -0.5, 0.109375, ((0, 2),))
    w_out_attn = normal_values(keys[15], (HEADS * VDIM, D), (HEADS * VDIM // 4) ** -0.5, 0.25, ((0, 2),))
    return {"tokens": tokens, "mix_gain": mix_gain, "w_pool_in": w_pool_in, "w_qlat": w_qlat, "w_kvlat": w_kvlat, "w_krope": w_krope, "q_gain": q_gain, "kv_gain": kv_gain, "w_q_content": w_q_content, "w_q_rotary": w_q_rotary, "w_key": w_key, "w_value": w_value, "pool_mix": pool_mix, "pool_scale": pool_scale, "w_out_pool": w_out_pool, "w_out_attn": w_out_attn}


eps_norm = 1e-06
rope_base = 10000.0
masked_score = -1e+30

def tables(positions, rotary_width):
    half_width = rotary_width // 2
    frequency = rope_base ** (-jnp.arange(half_width, dtype=jnp.float32) * 2.0 / rotary_width)
    angles = positions.astype(jnp.float32)[:, None] * frequency[None, :]
    return (jnp.cos(angles), jnp.sin(angles))

def rotate(vectors, cosine, sine_table):
    half_width = vectors.shape[-1] // 2
    first_half = vectors[..., :half_width]
    second_half = vectors[..., half_width:]
    return jnp.concatenate([first_half * cosine - second_half * sine_table, second_half * cosine + first_half * sine_table], axis=-1)

def latent_norm(latent, gain_vector):
    latent_values = latent.astype(jnp.float32)
    inverse = lax.rsqrt(lax.optimization_barrier(jnp.mean(latent_values * latent_values, axis=-1, keepdims=True)) + eps_norm)
    return (latent_values * inverse * gain_vector).astype(jnp.bfloat16)

def one_sequence(seq_tokens, mix_gain, w_pool_in, w_qlat, w_kvlat, w_krope, q_gain, kv_gain, w_q_content, w_q_rotary, w_key, w_value, pool_mix, pool_scale, w_out_pool, w_out_attn):
    length = seq_tokens.shape[0]
    positions = jnp.arange(length, dtype=jnp.int32)
    raw_values = seq_tokens.astype(jnp.float32)
    inverse_rms = lax.rsqrt(lax.optimization_barrier(jnp.mean(raw_values * raw_values, axis=1, keepdims=True)) + eps_norm)
    scaled = (raw_values * mix_gain).astype(jnp.bfloat16)

    def project(weight):
        return (jnp.dot(scaled, weight, preferred_element_type=jnp.float32) * inverse_rms).astype(jnp.bfloat16)
    pool_pre = project(w_pool_in)
    query_latent = project(w_qlat)
    kv_latent = project(w_kvlat)
    rotary_raw = project(w_krope)
    query_normed = latent_norm(query_latent, q_gain)
    key_normed = latent_norm(kv_latent, kv_gain)
    cosine, sine_table = tables(positions, ROPE)
    query_content = jnp.dot(query_normed, w_q_content, preferred_element_type=jnp.float32).astype(jnp.bfloat16).reshape(length, HEADS, NOPE)
    key_content = jnp.dot(key_normed, w_key, preferred_element_type=jnp.float32).astype(jnp.bfloat16).reshape(length, HEADS, NOPE)
    values = jnp.dot(key_normed, w_value, preferred_element_type=jnp.float32).astype(jnp.bfloat16).reshape(length, HEADS, VDIM)
    query_rotary = rotate(jnp.dot(query_normed, w_q_rotary, preferred_element_type=jnp.float32).reshape(length, HEADS, ROPE), cosine[:, None, :], sine_table[:, None, :]).astype(jnp.bfloat16)
    key_rotary = rotate(rotary_raw.astype(jnp.float32), cosine, sine_table).astype(jnp.bfloat16)
    score_scale = (NOPE + ROPE) ** (-0.5)
    key_content_wide = key_content.astype(jnp.float32)
    key_rotary_wide = key_rotary.astype(jnp.float32)
    values_wide = values.astype(jnp.float32)

    def query_block(block_index):
        row_start = block_index * TOK_DEV
        block_content = lax.dynamic_slice_in_dim(query_content, row_start, TOK_DEV, 0).astype(jnp.float32)
        block_rotary = lax.dynamic_slice_in_dim(query_rotary, row_start, TOK_DEV, 0).astype(jnp.float32)
        scores = jnp.einsum('qhd,khd->qhk', block_content, key_content_wide, precision=lax.Precision.HIGHEST)
        scores = scores + jnp.einsum('qhr,kr->qhk', block_rotary, key_rotary_wide, precision=lax.Precision.HIGHEST)
        query_positions = row_start + jnp.arange(TOK_DEV, dtype=jnp.int32)
        allowed = positions[None, None, :] <= query_positions[:, None, None]
        scores = jnp.where(allowed, scores * score_scale, masked_score)
        row_max = lax.optimization_barrier(jnp.max(scores, axis=-1))
        expo = jnp.exp(scores - row_max[..., None])
        row_total = lax.optimization_barrier(jnp.sum(expo, axis=-1))
        weights = lax.optimization_barrier(expo.astype(jnp.bfloat16))
        summed = jnp.einsum('qhk,khd->qhd', weights.astype(jnp.float32), values_wide, precision=lax.Precision.HIGHEST)
        attended = (summed / row_total[..., None]).astype(jnp.bfloat16).reshape(TOK_DEV, HEADS * VDIM)
        return (attended, row_max + jnp.log(row_total))
    attended, log_total = lax.map(query_block, jnp.arange(length // TOK_DEV))
    attended = attended.reshape(length, HEADS * VDIM)
    log_total = log_total.reshape(length, HEADS)
    pool_values = pool_pre.astype(jnp.float32)
    extended = jnp.concatenate([jnp.zeros((WIDEST - 1, POOL), jnp.float32), pool_values], axis=0)
    groups = jnp.arange(POOL, dtype=jnp.int32) // GROUP_DIM
    windows = jnp.left_shift(jnp.int32(2), groups % 4)
    window_sums = jnp.zeros((length, POOL), jnp.float32)
    for distance in range(WIDEST):
        window_sums = window_sums + jnp.where(distance < windows[None, :], extended[WIDEST - 1 - distance:WIDEST - 1 - distance + length], 0.0)
    counts = jnp.minimum(positions[:, None] + 1, windows[None, :]).astype(jnp.float32)
    pooled = lax.optimization_barrier((window_sums / counts - pool_values).astype(jnp.bfloat16))
    mixed_pool = jnp.einsum('sgc,gcd->sgd', pooled.astype(jnp.float32).reshape(length, GROUPS, GROUP_DIM), pool_mix.astype(jnp.float32), precision=lax.Precision.HIGHEST).reshape(length, POOL)
    pool_out = (mixed_pool * pool_scale).astype(jnp.bfloat16)
    layer_out = jnp.dot(pool_out, w_out_pool, preferred_element_type=jnp.float32)
    layer_out = layer_out + jnp.dot(attended, w_out_attn, preferred_element_type=jnp.float32)
    return (layer_out.astype(jnp.bfloat16), log_total)

def reference(tokens, mix_gain, w_pool_in, w_qlat, w_kvlat, w_krope, q_gain, kv_gain, w_q_content, w_q_rotary, w_key, w_value, pool_mix, pool_scale, w_out_pool, w_out_attn):
    sequences = tokens.reshape(SPAN, SEQS, TOK_DEV, D).transpose(1, 0, 2, 3).reshape(SEQS, SEQ_LEN, D)

    def per_sequence(seq_tokens):
        return one_sequence(seq_tokens, mix_gain, w_pool_in, w_qlat, w_kvlat, w_krope, q_gain, kv_gain, w_q_content, w_q_rotary, w_key, w_value, pool_mix, pool_scale, w_out_pool, w_out_attn)
    outputs, log_sums = lax.map(per_sequence, sequences)
    outputs = outputs.reshape(SEQS, SPAN, TOK_DEV, D).transpose(1, 0, 2, 3).reshape(TOKENS, D)
    log_sums = log_sums.reshape(SEQS, SPAN, TOK_DEV, HEADS).transpose(1, 0, 2, 3).reshape(TOKENS, HEADS)
    return (outputs, log_sums)
```

```python
import math

import jax
import jax.numpy as jnp
from jax import lax
from jax.experimental import pallas as pl
from jax.experimental.pallas import tpu as pltpu
from jax.sharding import PartitionSpec as P

NOPE = 128
ROPE = 64
VDIM = 128
GROUP_DIM = 128
WIDEST = 16
SPAN = 16


eps_norm = 1e-06
rope_base = 10000.0
masked_score = -1e30


def shifted(value, axis, steps):
    count = lax.axis_size(axis)
    leading, last = (max(0, -steps), min(count, count - steps))
    return lax.ppermute(value, axis, [(source, source + steps) for source in range(leading, last)])


def tables(positions, rotary_width):
    half_width = rotary_width // 2
    frequency = rope_base ** (-jnp.arange(half_width, dtype=jnp.float32) * 2.0 / rotary_width)
    angles = positions.astype(jnp.float32)[:, None] * frequency[None, :]
    return (jnp.cos(angles), jnp.sin(angles))


def rotate(vectors, cosine, sine_table):
    half_width = vectors.shape[-1] // 2
    first_half = vectors[..., :half_width]
    second_half = vectors[..., half_width:]
    return jnp.concatenate(
        [
            first_half * cosine - second_half * sine_table,
            second_half * cosine + first_half * sine_table,
        ],
        axis=-1,
    )


def latent_norm(latent, gain_vector):
    latent_values = latent.astype(jnp.float32)
    inverse = lax.rsqrt(jnp.mean(latent_values * latent_values, axis=-1, keepdims=True) + eps_norm)
    return (latent_values * inverse * gain_vector).astype(jnp.bfloat16)


def attend_kernel(
    rank_ref, query_ref, latent_ref, rotary_ref, w_key_ref, w_value_ref, out_ref, log_ref,
    key_scr, value_scr, peak_scr, total_scr, sum_scr,
):
    heads, rows, depth = query_ref.shape
    pair = 2 * rows
    scale = (NOPE + ROPE) ** (-0.5)
    factor = scale * math.log2(math.e)
    rank = rank_ref[0]

    def turn(first_block, initial):
        start = pl.multiple_of(jnp.maximum(first_block, 0) * rows, rows)
        latent = latent_ref[pl.ds(start, pair), :]
        rotary = rotary_ref[pl.ds(start, pair), :]
        if initial:
            row = lax.broadcasted_iota(jnp.int32, (rows, pair), 0) + rank * rows
            column = lax.broadcasted_iota(jnp.int32, (rows, pair), 1) + start
            allowed = (column <= row) & (column >= lower * rows)
        for head in range(heads):
            cols = slice(head * NOPE, (head + 1) * NOPE)
            key_scr[head, :, :NOPE] = jnp.dot(
                latent, w_key_ref[:, cols], preferred_element_type=jnp.float32
            ).astype(jnp.bfloat16)
            key_scr[head, :, NOPE:] = rotary
            value_scr[head] = jnp.dot(
                latent, w_value_ref[:, cols], preferred_element_type=jnp.float32
            ).astype(jnp.bfloat16)
        for head in range(heads):
            scores = lax.dot_general(
                query_ref[head], key_scr[head], (((1,), (1,)), ((), ())),
                preferred_element_type=jnp.float32,
            )
            if initial:
                scores = jnp.where(allowed, scores, masked_score)
                peak = jnp.max(scores, axis=1, keepdims=True)
            else:
                old = peak_scr[head][:, :1]
                peak = jnp.maximum(old, jnp.max(scores, axis=1, keepdims=True))
            expo = jnp.exp2((scores - peak) * factor)
            total = jnp.sum(expo, axis=1, keepdims=True)
            summed = jnp.dot(
                expo.astype(jnp.bfloat16), value_scr[head], preferred_element_type=jnp.float32
            )
            if not initial:
                shrink = jnp.exp2((old - peak) * factor)
                total = total + total_scr[head][:, :1] * shrink
                summed = summed + sum_scr[head] * shrink
            peak_scr[head] = jnp.broadcast_to(peak, (rows, 128))
            total_scr[head] = jnp.broadcast_to(total, (rows, 128))
            sum_scr[head] = summed

    odd = rank % 2
    lower = rank - odd
    first = jnp.maximum(rank - 1, 0)
    turn(first, True)

    def body(index, unused):
        turn(2 * index, False)
        return unused

    lax.fori_loop(0, rank // 2, body, 0)
    for head in range(heads):
        total = total_scr[head]
        out_ref[:, head * VDIM : (head + 1) * VDIM] = (sum_scr[head] / total).astype(jnp.bfloat16)
        log_ref[head] = (peak_scr[head] * scale + jnp.log(total))


def attention(rank, query, latent, rotary, w_key, w_value):
    heads, rows, depth = query.shape
    vmem = pl.BlockSpec(memory_space=pltpu.VMEM)
    return pl.pallas_call(
        attend_kernel,
        out_shape=(
            jax.ShapeDtypeStruct((rows, heads * VDIM), jnp.bfloat16),
            jax.ShapeDtypeStruct((heads, rows, 128), jnp.float32),
        ),
        in_specs=[pl.BlockSpec(memory_space=pltpu.SMEM)] + [vmem] * 5,
        out_specs=(vmem, vmem),
        scratch_shapes=[
            pltpu.VMEM((heads, 2 * rows, 2 * NOPE), jnp.bfloat16),
            pltpu.VMEM((heads, 2 * rows, VDIM), jnp.bfloat16),
            pltpu.VMEM((heads, rows, 128), jnp.float32),
            pltpu.VMEM((heads, rows, 128), jnp.float32),
            pltpu.VMEM((heads, rows, VDIM), jnp.float32),
        ],
        compiler_params=pltpu.CompilerParams(vmem_limit_bytes=60000 * 1024),
        cost_estimate=pl.CostEstimate(
            flops=20 * 10**9, bytes_accessed=10**7, transcendentals=10**7
        ),
    )(rank, query, latent, rotary, w_key, w_value)


def per_device(
    tokens,
    mix_gain,
    w_pool_in,
    w_qlat,
    w_kvlat,
    w_krope,
    q_gain,
    kv_gain,
    w_q_content,
    w_q_rotary,
    w_key,
    w_value,
    pool_mix,
    pool_scale,
    w_out_pool,
    w_out_attn,
):
    tp_size = lax.axis_size("tp")
    tp_rank = lax.axis_index("tp")
    sp_rank = lax.axis_index("sp")
    seq_count = lax.axis_size("sp") // SPAN
    local_rows, own_width = tokens.shape
    model_width = own_width * tp_size
    seq_rank = sp_rank // seq_count
    pool_cols = w_pool_in.shape[1]
    query_cols = w_qlat.shape[1]
    latent_cols = w_kvlat.shape[1]
    weight_cat = jnp.concatenate([w_pool_in, w_qlat, w_kvlat, w_krope], axis=1)
    raw_values = tokens.astype(jnp.float32)
    own_gain = lax.dynamic_slice_in_dim(mix_gain, tp_rank * own_width, own_width)
    squares = lax.psum(jnp.sum(raw_values * raw_values, axis=1), "tp")
    scaled = (raw_values * own_gain).astype(jnp.bfloat16)
    projected = jnp.dot(
        lax.all_gather(scaled, "tp", axis=1, tiled=True),
        weight_cat,
        preferred_element_type=jnp.float32,
    )
    inverse_rms = lax.rsqrt(squares / model_width + eps_norm)
    projected = (projected * inverse_rms[:, None]).astype(jnp.bfloat16)
    pool_pre = projected[:, :pool_cols]
    query_part = projected[:, pool_cols : pool_cols + query_cols]
    latent_part = projected[:, pool_cols + query_cols : pool_cols + query_cols + latent_cols]
    rotary_raw = projected[:, pool_cols + query_cols + latent_cols :]
    query_latent, kv_latent = (
        lax.all_gather(query_part, "tp", axis=1, tiled=True),
        lax.all_gather(latent_part, "tp", axis=1, tiled=True),
    )
    positions = seq_rank * local_rows + jnp.arange(local_rows, dtype=jnp.int32)
    query_normed = latent_norm(query_latent, q_gain)
    key_normed = latent_norm(kv_latent, kv_gain)
    own_heads = w_key.shape[1] // NOPE
    cosine, sine_table = tables(positions, ROPE)
    query_content = (
        jnp.dot(query_normed, w_q_content, preferred_element_type=jnp.float32)
        .astype(jnp.bfloat16)
        .reshape(local_rows, own_heads, NOPE)
    )
    query_rotary = rotate(
        jnp.dot(query_normed, w_q_rotary, preferred_element_type=jnp.float32).reshape(
            local_rows, own_heads, ROPE
        ),
        cosine[:, None, :],
        sine_table[:, None, :],
    ).astype(jnp.bfloat16)
    key_rotary = rotate(rotary_raw.astype(jnp.float32), cosine, sine_table).astype(jnp.bfloat16)
    query = jnp.concatenate(
        [
            query_content,
            query_rotary,
            jnp.zeros((local_rows, own_heads, 2 * NOPE - NOPE - ROPE), jnp.bfloat16),
        ],
        axis=-1,
    ).transpose(1, 0, 2)
    sequences = [
        [block * seq_count + sequence for block in range(SPAN)] for sequence in range(seq_count)
    ]
    packed = jnp.concatenate(
        [key_normed, key_rotary, jnp.zeros((local_rows, NOPE - ROPE), jnp.bfloat16)], axis=1
    )
    packed = lax.all_gather(packed, "sp", axis=0, tiled=True, axis_index_groups=sequences)
    latent_width = key_normed.shape[1]
    attended, log_wide = attention(
        seq_rank.astype(jnp.int32).reshape(1),
        query,
        packed[:, :latent_width],
        packed[:, latent_width:],
        w_key,
        w_value,
    )
    log_total = log_wide[:, :, 0].T
    group_count = pool_cols // GROUP_DIM
    rim_rows = shifted(pool_pre[local_rows - (WIDEST - 1) :], "sp", seq_count)
    rim_rows = jnp.where(seq_rank > 0, rim_rows, jnp.zeros_like(rim_rows))
    pool_values = pool_pre.astype(jnp.float32)
    extended = jnp.concatenate([rim_rows.astype(jnp.float32), pool_values], axis=0)
    groups = tp_rank * group_count + jnp.arange(pool_cols, dtype=jnp.int32) // GROUP_DIM
    windows = jnp.left_shift(jnp.int32(2), groups % 4)
    window_sums = jnp.zeros((local_rows, pool_cols), jnp.float32)
    for distance in range(WIDEST):
        window_sums = window_sums + jnp.where(
            distance < windows[None, :],
            extended[WIDEST - 1 - distance : WIDEST - 1 - distance + local_rows],
            0.0,
        )
    counts = jnp.minimum(positions[:, None] + 1, windows[None, :]).astype(jnp.float32)
    pooled = (window_sums / counts - pool_values).astype(jnp.bfloat16)
    own_mix = lax.dynamic_slice_in_dim(pool_mix, tp_rank * group_count, group_count, 0)
    mixed_pool = jnp.einsum(
        "rgc,gcd->rgd",
        pooled.reshape(local_rows, group_count, GROUP_DIM),
        own_mix,
        preferred_element_type=jnp.float32,
    ).reshape(local_rows, pool_cols)
    own_scale = lax.dynamic_slice_in_dim(pool_scale, tp_rank * pool_cols, pool_cols)
    pool_out = (mixed_pool * own_scale).astype(jnp.bfloat16)
    layer_out = lax.psum_scatter(
        (
            jnp.dot(pool_out, w_out_pool, preferred_element_type=jnp.float32)
            + jnp.dot(attended, w_out_attn, preferred_element_type=jnp.float32)
        ).astype(jnp.bfloat16),
        "tp",
        scatter_dimension=0,
        tiled=True,
    )
    return (layer_out, log_total)


def solution(mesh):
    in_specs = (
        P("sp", "tp"),
        P(),
        P(None, "tp"),
        P(None, "tp"),
        P(None, "tp"),
        P(),
        P(),
        P(),
        P(None, "tp"),
        P(None, "tp"),
        P(None, "tp"),
        P(None, "tp"),
        P(),
        P(),
        P("tp", None),
        P("tp", None),
    )
    out_specs = (P(("sp", "tp"), None), P("sp", "tp"))
    return jax.shard_map(
        per_device, mesh=mesh, in_specs=in_specs, out_specs=out_specs, check_vma=False
    )
```

```python
import functools
import math

import jax
import jax.numpy as jnp
from jax import lax
from jax.experimental import pallas as pl
from jax.experimental.pallas import tpu as pltpu
from jax.sharding import PartitionSpec as P

NOPE = 128
ROPE = 64
VDIM = 128
GROUP_DIM = 128
WIDEST = 16
SPAN = 16
MESH = pl.DeviceIdType.MESH


eps_norm = 1e-06
rope_base = 10000.0
masked_score = -1e30


def shifted(value, axis, steps):
    count = lax.axis_size(axis)
    leading, last = (max(0, -steps), min(count, count - steps))
    return lax.ppermute(value, axis, [(source, source + steps) for source in range(leading, last)])


def tables(positions, rotary_width):
    half_width = rotary_width // 2
    frequency = rope_base ** (-jnp.arange(half_width, dtype=jnp.float32) * 2.0 / rotary_width)
    angles = positions.astype(jnp.float32)[:, None] * frequency[None, :]
    return (jnp.cos(angles), jnp.sin(angles))


def rotate(vectors, cosine, sine_table):
    half_width = vectors.shape[-1] // 2
    first_half = vectors[..., :half_width]
    second_half = vectors[..., half_width:]
    return jnp.concatenate(
        [
            first_half * cosine - second_half * sine_table,
            second_half * cosine + first_half * sine_table,
        ],
        axis=-1,
    )


def latent_norm(latent, gain_vector):
    latent_values = latent.astype(jnp.float32)
    inverse = lax.rsqrt(jnp.mean(latent_values * latent_values, axis=-1, keepdims=True) + eps_norm)
    return (latent_values * inverse * gain_vector).astype(jnp.bfloat16)


QUAD = 4


def attend_kernel(
    seq_count, tp_size, query_ref, packed_ref, w_key_ref, w_value_ref, out_ref, log_ref,
    blocks, queries, peak_scr, total_scr, sum_scr, give, take, log_give, log_take,
    ici_recv, core_recv, z_send, near_send, far_send, core_send, swap_send, swap_recv,
):
    heads, rows, depth = query_ref.shape
    half_heads = heads // 2
    own_width = half_heads * NOPE
    latent_width = w_key_ref.shape[0]
    layers = SPAN // QUAD
    scale = (NOPE + ROPE) ** (-0.5)
    factor = scale * math.log2(math.e)
    part = rows // tp_size

    place = lax.axis_index("sp")
    core = lax.axis_index("tp")
    sequence = place % seq_count
    rank = place // seq_count
    z, y, x = rank // QUAD, (rank % QUAD) // 2, rank % 2
    low = jnp.minimum(rank, SPAN - 1 - rank)
    high = SPAN - 1 - low
    side = rank // (SPAN // 2)
    near_x, near_y = 1 - core % 2, core % 2
    far_x, far_y = core % 2, 1 - core % 2

    def block_at(up, step_x, step_y):
        return ((z + up) % layers) * QUAD + ((y + step_y) % 2) * 2 + (x + step_x) % 2

    def device(block, which_core):
        return (block * seq_count + sequence, which_core)

    near = block_at(0, near_x, near_y)
    far = block_at(0, far_x, far_y)
    mate = SPAN - 1 - rank
    siblings = [(core + step) % tp_size for step in range(1, tp_size)]
    friends = [device(block_at(up, 0, 0), core) for up in range(1, layers)]
    friends += [device(near, core), device(far, core), device(mate, core)]
    friends += [device(rank, sibling) for sibling in siblings]

    barrier = pltpu.get_barrier_semaphore()
    for friend in friends:
        pl.semaphore_signal(barrier, inc=1, device_id=friend, device_id_type=MESH)
    pl.semaphore_wait(barrier, len(friends))

    def piece(block, owner):
        return blocks.at[block, pl.ds(pl.multiple_of(owner * part, part), part), :]

    def remote(source, target, send, recv, where):
        return pltpu.make_async_remote_copy(
            src_ref=source, dst_ref=target, send_sem=send, recv_sem=recv,
            device_id=where, device_id_type=MESH,
        )

    def ici(source, block, send, where):
        return remote(source, piece(block, core), send, ici_recv.at[block], where)

    def across(block, step):
        return remote(
            piece(block, core), piece(block, core), core_send.at[block, step - 1],
            core_recv.at[block, step - 1], device(rank, (core + step) % tp_size),
        )

    def arrival(block, step):
        giver = (core + tp_size - step) % tp_size
        return remote(
            piece(block, giver), piece(block, giver), core_send.at[block, step - 1],
            core_recv.at[block, step - 1], device(rank, giver),
        )

    def swap(source, target, index):
        return remote(source, target, swap_send.at[index], swap_recv.at[index], device(mate, core))

    give_heads = pl.ds((1 - side) * half_heads, half_heads)
    own_rows = pl.ds(pl.multiple_of(side * rows, rows), rows)
    mate_rows = pl.ds(pl.multiple_of((1 - side) * rows, rows), rows)
    swap(query_ref.at[give_heads], queries.at[:, own_rows, :], 0).start()
    own_piece = packed_ref.at[pl.ds(pl.multiple_of(core * part, part), part), :]
    for up in range(1, layers):
        ici(own_piece, rank, z_send.at[up - 1], device(block_at(up, 0, 0), core)).start()
    ici(own_piece, rank, near_send.at[0], device(near, core)).start()
    ici(own_piece, rank, far_send.at[0], device(far, core)).start()

    blocks[rank] = packed_ref[...]
    for head in range(half_heads):
        queries[head, own_rows, :] = query_ref[side * half_heads + head]
    peak_scr[...] = jnp.full(peak_scr.shape, masked_score, jnp.float32)
    total_scr[...] = jnp.zeros_like(total_scr)
    sum_scr[...] = jnp.zeros_like(sum_scr)

    def landed(block):
        ici(piece(block, core), block, near_send.at[0], device(near, core)).wait_recv()

    def hand_over(block):
        for step in range(1, tp_size):
            across(block, step).start()

    def pump(turn):
        group, up = turn // layers, turn % layers

        @pl.when(group == 0)
        def _():
            block = block_at(up, 0, 0)
            landed(block)
            ici(piece(block, core), block, near_send.at[up], device(near, core)).start()
            ici(piece(block, core), block, far_send.at[up], device(far, core)).start()
            hand_over(block)

        @pl.when(group == 1)
        def _():
            block = block_at(up, near_x, near_y)
            landed(block)
            ici(piece(block, core), block, far_send.at[layers + up], device(far, core)).start()
            hand_over(block)
            other = block_at(up, far_x, far_y)
            landed(other)
            hand_over(other)

        @pl.when(group == 3)
        def _():
            block = block_at(up, 1, 1)
            landed(block)
            hand_over(block)

    own_cols = pl.ds(pl.multiple_of(side * own_width, own_width), own_width)

    def unit(block, both, masked):
        held = slice(0, 2 * rows) if both else slice(rows, 2 * rows)
        count = 2 * rows if both else rows
        latent = blocks[block, :, :latent_width]
        rotary = blocks[block, :, latent_width:]
        keys = jnp.dot(
            latent, w_key_ref[:, own_cols], preferred_element_type=jnp.float32
        ).astype(jnp.bfloat16)
        values = jnp.dot(
            latent, w_value_ref[:, own_cols], preferred_element_type=jnp.float32
        ).astype(jnp.bfloat16)
        if masked:
            row = lax.broadcasted_iota(jnp.int32, (count, rows), 0)
            column = lax.broadcasted_iota(jnp.int32, (count, rows), 1)
            allowed = column <= row
        for head in range(half_heads):
            cols = slice(head * NOPE, (head + 1) * NOPE)
            scores = lax.dot_general(
                queries[head, held, :],
                jnp.concatenate([keys[:, cols], rotary], axis=1),
                (((1,), (1,)), ((), ())),
                preferred_element_type=jnp.float32,
            )
            if masked:
                scores = jnp.where(allowed, scores, masked_score)
            old = peak_scr[head, held, :1]
            peak = jnp.maximum(old, jnp.max(scores, axis=1, keepdims=True))
            expo = jnp.exp2((scores - peak) * factor)
            shrink = jnp.exp2((old - peak) * factor)
            total = total_scr[head, held, :1] * shrink + jnp.sum(expo, axis=1, keepdims=True)
            summed = jnp.dot(
                expo.astype(jnp.bfloat16), values[:, cols], preferred_element_type=jnp.float32
            )
            sum_scr[head, held, :] = sum_scr[head, held, :] * shrink + summed
            peak_scr[head, held, :] = jnp.broadcast_to(peak, (count, 128))
            total_scr[head, held, :] = jnp.broadcast_to(total, (count, 128))

    swap(query_ref.at[give_heads], queries.at[:, mate_rows, :], 0).wait_recv()

    def turn_body(turn, unused):
        group, up = turn // layers, turn % layers
        block = block_at(up, group % 2, group // 2)

        @pl.when(turn >= 1)
        def _():
            @pl.when(turn < SPAN - 1)
            def _():
                pump(turn + 1)

            for step in range(1, tp_size):
                arrival(block, step).wait_recv()

        @pl.when(block < low)
        def _():
            unit(block, True, False)

        @pl.when(block == low)
        def _():
            unit(block, True, True)

        @pl.when((block > low) & (block < high))
        def _():
            unit(block, False, False)

        @pl.when(block == high)
        def _():
            unit(block, False, True)

        @pl.when(turn == 0)
        def _():
            pump(turn + 1)

        return unused

    lax.fori_loop(0, SPAN, turn_body, 0)

    lane = lax.broadcasted_iota(jnp.int32, (rows, 128), 1)

    def finish(which):
        logs = jnp.zeros((rows, 128), jnp.float32)
        pieces = []
        for head in range(half_heads):
            total = total_scr[head, which, :]
            pieces.append((sum_scr[head, which, :] / total).astype(jnp.bfloat16))
            logs = jnp.where(lane == head, peak_scr[head, which, :] * scale + jnp.log(total), logs)
        return jnp.concatenate(pieces, axis=1), jnp.transpose(logs)[: log_give.shape[0]]

    give[...], log_give[...] = finish(mate_rows)
    swap(give, take, 1).start()
    swap(log_give, log_take, 2).start()
    attended, logs = finish(own_rows)
    out_ref[:, own_cols] = attended
    log_ref[side] = logs
    swap(give, take, 1).wait_recv()
    swap(log_give, log_take, 2).wait_recv()
    mate_cols = pl.ds(pl.multiple_of((1 - side) * own_width, own_width), own_width)
    out_ref[:, mate_cols] = take[...]
    log_ref[1 - side] = log_take[...]

    swap(query_ref.at[give_heads], queries.at[:, own_rows, :], 0).wait_send()
    swap(give, take, 1).wait_send()
    swap(log_give, log_take, 2).wait_send()
    for up in range(1, layers):
        ici(own_piece, rank, z_send.at[up - 1], device(near, core)).wait_send()
    for up in range(layers):
        ici(own_piece, rank, near_send.at[up], device(near, core)).wait_send()
    for up in range(2 * layers):
        ici(own_piece, rank, far_send.at[up], device(far, core)).wait_send()

    def drain(turn, unused):
        group, up = turn // layers, turn % layers
        block = block_at(up, group % 2, group // 2)
        for step in range(1, tp_size):
            across(block, step).wait_send()
        return unused

    lax.fori_loop(1, SPAN, drain, 0)


def attention(seq_count, tp_size, query, packed, w_key, w_value):
    heads, rows, depth = query.shape
    half = heads // 2
    padded = -(-half // 8) * 8
    vmem = pl.BlockSpec(memory_space=pltpu.VMEM)
    dma = pltpu.SemaphoreType.DMA
    return pl.pallas_call(
        functools.partial(attend_kernel, seq_count, tp_size),
        out_shape=(
            jax.ShapeDtypeStruct((rows, heads * VDIM), jnp.bfloat16),
            jax.ShapeDtypeStruct((2, padded, rows), jnp.float32),
        ),
        in_specs=[vmem] * 4,
        out_specs=(vmem, vmem),
        scratch_shapes=[
            pltpu.VMEM((SPAN,) + packed.shape, jnp.bfloat16),
            pltpu.VMEM((half, 2 * rows, depth), jnp.bfloat16),
            pltpu.VMEM((half, 2 * rows, 128), jnp.float32),
            pltpu.VMEM((half, 2 * rows, 128), jnp.float32),
            pltpu.VMEM((half, 2 * rows, VDIM), jnp.float32),
            pltpu.VMEM((rows, half * VDIM), jnp.bfloat16),
            pltpu.VMEM((rows, half * VDIM), jnp.bfloat16),
            pltpu.VMEM((padded, rows), jnp.float32),
            pltpu.VMEM((padded, rows), jnp.float32),
            dma((SPAN,)),
            dma((SPAN, tp_size - 1)),
            dma((SPAN // QUAD - 1,)),
            dma((SPAN // QUAD,)),
            dma((2 * SPAN // QUAD,)),
            dma((SPAN, tp_size - 1)),
            dma((3,)),
            dma((3,)),
        ],
        compiler_params=pltpu.CompilerParams(
            vmem_limit_bytes=56000 * 1024, collective_id=0, has_side_effects=True
        ),
        cost_estimate=pl.CostEstimate(
            flops=20 * 10**9, bytes_accessed=10**7, transcendentals=10**7
        ),
    )(query, packed, w_key, w_value)


def per_device(
    tokens,
    mix_gain,
    w_pool_in,
    w_qlat,
    w_kvlat,
    w_krope,
    q_gain,
    kv_gain,
    w_q_content,
    w_q_rotary,
    w_key,
    w_value,
    pool_mix,
    pool_scale,
    w_out_pool,
    w_out_attn,
):
    tp_size = lax.axis_size("tp")
    tp_rank = lax.axis_index("tp")
    sp_rank = lax.axis_index("sp")
    seq_count = lax.axis_size("sp") // SPAN
    local_rows, own_width = tokens.shape
    model_width = own_width * tp_size
    seq_rank = sp_rank // seq_count
    pool_cols = w_pool_in.shape[1]
    query_cols = w_qlat.shape[1]
    latent_cols = w_kvlat.shape[1]
    weight_cat = jnp.concatenate([w_pool_in, w_qlat, w_kvlat, w_krope], axis=1)
    raw_values = tokens.astype(jnp.float32)
    own_gain = lax.dynamic_slice_in_dim(mix_gain, tp_rank * own_width, own_width)
    squares = lax.psum(jnp.sum(raw_values * raw_values, axis=1), "tp")
    scaled = (raw_values * own_gain).astype(jnp.bfloat16)
    projected = jnp.dot(
        lax.all_gather(scaled, "tp", axis=1, tiled=True),
        weight_cat,
        preferred_element_type=jnp.float32,
    )
    inverse_rms = lax.rsqrt(squares / model_width + eps_norm)
    projected = (projected * inverse_rms[:, None]).astype(jnp.bfloat16)
    pool_pre = projected[:, :pool_cols]
    query_part = projected[:, pool_cols : pool_cols + query_cols]
    latent_part = projected[:, pool_cols + query_cols : pool_cols + query_cols + latent_cols]
    rotary_raw = projected[:, pool_cols + query_cols + latent_cols :]
    query_latent, kv_latent = (
        lax.all_gather(query_part, "tp", axis=1, tiled=True),
        lax.all_gather(latent_part, "tp", axis=1, tiled=True),
    )
    positions = seq_rank * local_rows + jnp.arange(local_rows, dtype=jnp.int32)
    query_normed = latent_norm(query_latent, q_gain)
    key_normed = latent_norm(kv_latent, kv_gain)
    own_heads = w_key.shape[1] // NOPE
    cosine, sine_table = tables(positions, ROPE)
    query_content = (
        jnp.dot(query_normed, w_q_content, preferred_element_type=jnp.float32)
        .astype(jnp.bfloat16)
        .reshape(local_rows, own_heads, NOPE)
    )
    query_rotary = rotate(
        jnp.dot(query_normed, w_q_rotary, preferred_element_type=jnp.float32).reshape(
            local_rows, own_heads, ROPE
        ),
        cosine[:, None, :],
        sine_table[:, None, :],
    ).astype(jnp.bfloat16)
    key_rotary = rotate(rotary_raw.astype(jnp.float32), cosine, sine_table).astype(jnp.bfloat16)
    query = jnp.concatenate(
        [
            query_content,
            query_rotary,
            jnp.zeros((local_rows, own_heads, 2 * NOPE - NOPE - ROPE), jnp.bfloat16),
        ],
        axis=-1,
    ).transpose(1, 0, 2)
    packed = jnp.concatenate(
        [key_normed, key_rotary, jnp.zeros((local_rows, NOPE - ROPE), jnp.bfloat16)], axis=1
    )
    attended, log_rows = attention(seq_count, tp_size, query, packed, w_key, w_value)
    log_total = log_rows[:, : own_heads // 2].reshape(own_heads, local_rows).T
    group_count = pool_cols // GROUP_DIM
    rim_rows = shifted(pool_pre[local_rows - (WIDEST - 1) :], "sp", seq_count)
    rim_rows = jnp.where(seq_rank > 0, rim_rows, jnp.zeros_like(rim_rows))
    pool_values = pool_pre.astype(jnp.float32)
    extended = jnp.concatenate([rim_rows.astype(jnp.float32), pool_values], axis=0)
    groups = tp_rank * group_count + jnp.arange(pool_cols, dtype=jnp.int32) // GROUP_DIM
    windows = jnp.left_shift(jnp.int32(2), groups % 4)
    window_sums = jnp.zeros((local_rows, pool_cols), jnp.float32)
    for distance in range(WIDEST):
        window_sums = window_sums + jnp.where(
            distance < windows[None, :],
            extended[WIDEST - 1 - distance : WIDEST - 1 - distance + local_rows],
            0.0,
        )
    counts = jnp.minimum(positions[:, None] + 1, windows[None, :]).astype(jnp.float32)
    pooled = (window_sums / counts - pool_values).astype(jnp.bfloat16)
    own_mix = lax.dynamic_slice_in_dim(pool_mix, tp_rank * group_count, group_count, 0)
    mixed_pool = jnp.einsum(
        "rgc,gcd->rgd",
        pooled.reshape(local_rows, group_count, GROUP_DIM),
        own_mix,
        preferred_element_type=jnp.float32,
    ).reshape(local_rows, pool_cols)
    own_scale = lax.dynamic_slice_in_dim(pool_scale, tp_rank * pool_cols, pool_cols)
    pool_out = (mixed_pool * own_scale).astype(jnp.bfloat16)
    layer_out = lax.psum_scatter(
        (
            jnp.dot(pool_out, w_out_pool, preferred_element_type=jnp.float32)
            + jnp.dot(attended, w_out_attn, preferred_element_type=jnp.float32)
        ).astype(jnp.bfloat16),
        "tp",
        scatter_dimension=0,
        tiled=True,
    )
    return (layer_out, log_total)


def solution(mesh):
    in_specs = (
        P("sp", "tp"),
        P(),
        P(None, "tp"),
        P(None, "tp"),
        P(None, "tp"),
        P(),
        P(),
        P(),
        P(None, "tp"),
        P(None, "tp"),
        P(None, "tp"),
        P(None, "tp"),
        P(),
        P(),
        P("tp", None),
        P("tp", None),
    )
    out_specs = (P(("sp", "tp"), None), P("sp", "tp"))
    return jax.shard_map(
        per_device, mesh=mesh, in_specs=in_specs, out_specs=out_specs, check_vma=False
    )
```

```python
import functools
import math

import jax
import jax.numpy as jnp
from jax import lax
from jax.experimental import pallas as pl
from jax.experimental.pallas import tpu as pltpu
from jax.sharding import PartitionSpec as P

NOPE = 128
ROPE = 64
VDIM = 128
GROUP_DIM = 128
WIDEST = 16
SPAN = 16
MESH = pl.DeviceIdType.MESH


eps_norm = 1e-06
rope_base = 10000.0
masked_score = -1e30


def shifted(value, axis, steps):
    count = lax.axis_size(axis)
    leading, last = (max(0, -steps), min(count, count - steps))
    return lax.ppermute(value, axis, [(source, source + steps) for source in range(leading, last)])


def tables(positions, rotary_width):
    half_width = rotary_width // 2
    frequency = rope_base ** (-jnp.arange(half_width, dtype=jnp.float32) * 2.0 / rotary_width)
    angles = positions.astype(jnp.float32)[:, None] * frequency[None, :]
    return (jnp.cos(angles), jnp.sin(angles))


def rotate(vectors, cosine, sine_table):
    half_width = vectors.shape[-1] // 2
    first_half = vectors[..., :half_width]
    second_half = vectors[..., half_width:]
    return jnp.concatenate(
        [
            first_half * cosine - second_half * sine_table,
            second_half * cosine + first_half * sine_table,
        ],
        axis=-1,
    )


def latent_norm(latent, gain_vector):
    latent_values = latent.astype(jnp.float32)
    inverse = lax.rsqrt(jnp.mean(latent_values * latent_values, axis=-1, keepdims=True) + eps_norm)
    return (latent_values * inverse * gain_vector).astype(jnp.bfloat16)


QUAD = 4


def attend_kernel(
    seq_count, tp_size, query_ref, packed_ref, w_key_ref, w_value_ref, out_ref, log_ref,
    blocks, queries, peak_scr, total_scr, sum_scr, give, take, log_give, log_take,
    ici_recv, core_recv, z_send, near_send, far_send, core_send, swap_send, swap_recv,
):
    heads, rows, depth = query_ref.shape
    half_heads = heads // 2
    own_width = half_heads * NOPE
    latent_width = w_key_ref.shape[0]
    layers = SPAN // QUAD
    scale = (NOPE + ROPE) ** (-0.5)
    factor = scale * math.log2(math.e)
    part = rows // tp_size

    place = lax.axis_index("sp")
    core = lax.axis_index("tp")
    sequence = place % seq_count
    rank = place // seq_count
    z, y, x = rank // QUAD, (rank % QUAD) // 2, rank % 2
    low = jnp.minimum(rank, SPAN - 1 - rank)
    high = SPAN - 1 - low
    side = rank // (SPAN // 2)
    near_x, near_y = 1 - core % 2, core % 2
    far_x, far_y = core % 2, 1 - core % 2

    def block_at(up, step_x, step_y):
        return ((z + up) % layers) * QUAD + ((y + step_y) % 2) * 2 + (x + step_x) % 2

    def device(block, which_core):
        return (block * seq_count + sequence, which_core)

    near = block_at(0, near_x, near_y)
    far = block_at(0, far_x, far_y)
    mate = SPAN - 1 - rank
    siblings = [(core + step) % tp_size for step in range(1, tp_size)]
    friends = [device(block_at(up, 0, 0), core) for up in range(1, layers)]
    friends += [device(near, core), device(far, core), device(mate, core)]
    friends += [device(rank, sibling) for sibling in siblings]

    barrier = pltpu.get_barrier_semaphore()
    for friend in friends:
        pl.semaphore_signal(barrier, inc=1, device_id=friend, device_id_type=MESH)
    pl.semaphore_wait(barrier, len(friends))

    def piece(block, owner):
        return blocks.at[block, pl.ds(pl.multiple_of(owner * part, part), part), :]

    def remote(source, target, send, recv, where):
        return pltpu.make_async_remote_copy(
            src_ref=source, dst_ref=target, send_sem=send, recv_sem=recv,
            device_id=where, device_id_type=MESH,
        )

    def ici(source, block, send, where):
        return remote(source, piece(block, core), send, ici_recv.at[block], where)

    def across(block, step):
        return remote(
            piece(block, core), piece(block, core), core_send.at[block, step - 1],
            core_recv.at[block, step - 1], device(rank, (core + step) % tp_size),
        )

    def arrival(block, step):
        giver = (core + tp_size - step) % tp_size
        return remote(
            piece(block, giver), piece(block, giver), core_send.at[block, step - 1],
            core_recv.at[block, step - 1], device(rank, giver),
        )

    def swap(source, target, index):
        return remote(source, target, swap_send.at[index], swap_recv.at[index], device(mate, core))

    give_heads = pl.ds((1 - side) * half_heads, half_heads)
    own_rows = pl.ds(pl.multiple_of(side * rows, rows), rows)
    mate_rows = pl.ds(pl.multiple_of((1 - side) * rows, rows), rows)
    own_piece = packed_ref.at[pl.ds(pl.multiple_of(core * part, part), part), :]
    for up in range(1, layers):
        ici(own_piece, rank, z_send.at[up - 1], device(block_at(up, 0, 0), core)).start()
    ici(own_piece, rank, near_send.at[0], device(near, core)).start()
    ici(own_piece, rank, far_send.at[0], device(far, core)).start()

    swap(query_ref.at[give_heads], queries.at[:, own_rows, :], 0).start()

    blocks[rank] = packed_ref[...]
    for head in range(half_heads):
        queries[head, own_rows, :] = query_ref[side * half_heads + head]
    peak_scr[...] = jnp.full(peak_scr.shape, masked_score, jnp.float32)
    total_scr[...] = jnp.zeros_like(total_scr)
    sum_scr[...] = jnp.zeros_like(sum_scr)

    def landed(block):
        ici(piece(block, core), block, near_send.at[0], device(near, core)).wait_recv()

    def hand_over(block):
        for step in range(1, tp_size):
            across(block, step).start()

    def pump(turn):
        group, up = turn // layers, turn % layers

        @pl.when(group == 0)
        def _():
            block = block_at(up, 0, 0)
            landed(block)
            ici(piece(block, core), block, near_send.at[up], device(near, core)).start()
            ici(piece(block, core), block, far_send.at[up], device(far, core)).start()
            hand_over(block)

        @pl.when(group == 1)
        def _():
            block = block_at(up, near_x, near_y)
            landed(block)
            ici(piece(block, core), block, far_send.at[layers + up], device(far, core)).start()
            hand_over(block)
            other = block_at(up, far_x, far_y)
            landed(other)
            hand_over(other)

        @pl.when(group == 3)
        def _():
            block = block_at(up, 1, 1)
            landed(block)
            hand_over(block)

    own_cols = pl.ds(pl.multiple_of(side * own_width, own_width), own_width)

    def unit(block, both, masked):
        held = slice(0, 2 * rows) if both else slice(rows, 2 * rows)
        count = 2 * rows if both else rows
        latent = blocks[block, :, :latent_width]
        rotary = blocks[block, :, latent_width:]
        keys = jnp.dot(
            latent, w_key_ref[:, own_cols], preferred_element_type=jnp.float32
        ).astype(jnp.bfloat16)
        values = jnp.dot(
            latent, w_value_ref[:, own_cols], preferred_element_type=jnp.float32
        ).astype(jnp.bfloat16)
        if masked:
            row = lax.broadcasted_iota(jnp.int32, (count, rows), 0)
            column = lax.broadcasted_iota(jnp.int32, (count, rows), 1)
            allowed = column <= row
        for head in range(half_heads):
            cols = slice(head * NOPE, (head + 1) * NOPE)
            scores = lax.dot_general(
                queries[head, held, :],
                jnp.concatenate([keys[:, cols], rotary], axis=1),
                (((1,), (1,)), ((), ())),
                preferred_element_type=jnp.float32,
            )
            if masked:
                scores = jnp.where(allowed, scores, masked_score)
            old = peak_scr[head, held, :1]
            peak = jnp.maximum(old, jnp.max(scores, axis=1, keepdims=True))
            expo = jnp.exp2((scores - peak) * factor)
            shrink = jnp.exp2((old - peak) * factor)
            total = total_scr[head, held, :1] * shrink + jnp.sum(expo, axis=1, keepdims=True)
            summed = jnp.dot(
                expo.astype(jnp.bfloat16), values[:, cols], preferred_element_type=jnp.float32
            )
            sum_scr[head, held, :] = sum_scr[head, held, :] * shrink + summed
            peak_scr[head, held, :] = jnp.broadcast_to(peak, (count, 128))
            total_scr[head, held, :] = jnp.broadcast_to(total, (count, 128))

    for up in range(1, layers):
        pump(up)
    swap(query_ref.at[give_heads], queries.at[:, mate_rows, :], 0).wait_recv()

    def turn_body(turn, unused):
        group, up = turn // layers, turn % layers
        block = block_at(up, group % 2, group // 2)

        @pl.when(turn < SPAN - layers)
        def _():
            pump(turn + layers)

        @pl.when(turn >= 1)
        def _():
            for step in range(1, tp_size):
                arrival(block, step).wait_recv()

        @pl.when(block < low)
        def _():
            unit(block, True, False)

        @pl.when(block == low)
        def _():
            unit(block, True, True)

        @pl.when((block > low) & (block < high))
        def _():
            unit(block, False, False)

        @pl.when(block == high)
        def _():
            unit(block, False, True)

        return unused

    lax.fori_loop(0, SPAN, turn_body, 0)

    lane = lax.broadcasted_iota(jnp.int32, (rows, 128), 1)

    def finish(which):
        logs = jnp.zeros((rows, 128), jnp.float32)
        pieces = []
        for head in range(half_heads):
            total = total_scr[head, which, :]
            pieces.append((sum_scr[head, which, :] / total).astype(jnp.bfloat16))
            logs = jnp.where(lane == head, peak_scr[head, which, :] * scale + jnp.log(total), logs)
        return jnp.concatenate(pieces, axis=1), jnp.transpose(logs)[: log_give.shape[0]]

    give[...], log_give[...] = finish(mate_rows)
    swap(give, take, 1).start()
    swap(log_give, log_take, 2).start()
    attended, logs = finish(own_rows)
    out_ref[:, own_cols] = attended
    log_ref[side] = logs
    swap(give, take, 1).wait_recv()
    swap(log_give, log_take, 2).wait_recv()
    mate_cols = pl.ds(pl.multiple_of((1 - side) * own_width, own_width), own_width)
    out_ref[:, mate_cols] = take[...]
    log_ref[1 - side] = log_take[...]

    swap(query_ref.at[give_heads], queries.at[:, own_rows, :], 0).wait_send()
    swap(give, take, 1).wait_send()
    swap(log_give, log_take, 2).wait_send()
    for up in range(1, layers):
        ici(own_piece, rank, z_send.at[up - 1], device(near, core)).wait_send()
    for up in range(layers):
        ici(own_piece, rank, near_send.at[up], device(near, core)).wait_send()
    for up in range(2 * layers):
        ici(own_piece, rank, far_send.at[up], device(far, core)).wait_send()

    def drain(turn, unused):
        group, up = turn // layers, turn % layers
        block = block_at(up, group % 2, group // 2)
        for step in range(1, tp_size):
            across(block, step).wait_send()
        return unused

    lax.fori_loop(1, SPAN, drain, 0)


def attention(seq_count, tp_size, query, packed, w_key, w_value):
    heads, rows, depth = query.shape
    half = heads // 2
    padded = -(-half // 8) * 8
    vmem = pl.BlockSpec(memory_space=pltpu.VMEM)
    dma = pltpu.SemaphoreType.DMA
    return pl.pallas_call(
        functools.partial(attend_kernel, seq_count, tp_size),
        out_shape=(
            jax.ShapeDtypeStruct((rows, heads * VDIM), jnp.bfloat16),
            jax.ShapeDtypeStruct((2, padded, rows), jnp.float32),
        ),
        in_specs=[vmem] * 4,
        out_specs=(vmem, vmem),
        scratch_shapes=[
            pltpu.VMEM((SPAN,) + packed.shape, jnp.bfloat16),
            pltpu.VMEM((half, 2 * rows, depth), jnp.bfloat16),
            pltpu.VMEM((half, 2 * rows, 128), jnp.float32),
            pltpu.VMEM((half, 2 * rows, 128), jnp.float32),
            pltpu.VMEM((half, 2 * rows, VDIM), jnp.float32),
            pltpu.VMEM((rows, half * VDIM), jnp.bfloat16),
            pltpu.VMEM((rows, half * VDIM), jnp.bfloat16),
            pltpu.VMEM((padded, rows), jnp.float32),
            pltpu.VMEM((padded, rows), jnp.float32),
            dma((SPAN,)),
            dma((SPAN, tp_size - 1)),
            dma((SPAN // QUAD - 1,)),
            dma((SPAN // QUAD,)),
            dma((2 * SPAN // QUAD,)),
            dma((SPAN, tp_size - 1)),
            dma((3,)),
            dma((3,)),
        ],
        compiler_params=pltpu.CompilerParams(
            vmem_limit_bytes=56000 * 1024, collective_id=0, has_side_effects=True
        ),
        cost_estimate=pl.CostEstimate(
            flops=20 * 10**9, bytes_accessed=10**7, transcendentals=10**7
        ),
    )(query, packed, w_key, w_value)


def per_device(
    tokens,
    mix_gain,
    w_pool_in,
    w_qlat,
    w_kvlat,
    w_krope,
    q_gain,
    kv_gain,
    w_q_content,
    w_q_rotary,
    w_key,
    w_value,
    pool_mix,
    pool_scale,
    w_out_pool,
    w_out_attn,
):
    tp_size = lax.axis_size("tp")
    tp_rank = lax.axis_index("tp")
    sp_rank = lax.axis_index("sp")
    seq_count = lax.axis_size("sp") // SPAN
    local_rows, own_width = tokens.shape
    model_width = own_width * tp_size
    seq_rank = sp_rank // seq_count
    pool_cols = w_pool_in.shape[1]
    query_cols = w_qlat.shape[1]
    latent_cols = w_kvlat.shape[1]
    weight_cat = jnp.concatenate([w_pool_in, w_qlat, w_kvlat, w_krope], axis=1)
    raw_values = tokens.astype(jnp.float32)
    own_gain = lax.dynamic_slice_in_dim(mix_gain, tp_rank * own_width, own_width)
    squares = lax.psum(jnp.sum(raw_values * raw_values, axis=1), "tp")
    scaled = (raw_values * own_gain).astype(jnp.bfloat16)
    projected = jnp.dot(
        lax.all_gather(scaled, "tp", axis=1, tiled=True),
        weight_cat,
        preferred_element_type=jnp.float32,
    )
    inverse_rms = lax.rsqrt(squares / model_width + eps_norm)
    projected = (projected * inverse_rms[:, None]).astype(jnp.bfloat16)
    pool_pre = projected[:, :pool_cols]
    query_part = projected[:, pool_cols : pool_cols + query_cols]
    latent_part = projected[:, pool_cols + query_cols : pool_cols + query_cols + latent_cols]
    rotary_raw = projected[:, pool_cols + query_cols + latent_cols :]
    query_latent, kv_latent = (
        lax.all_gather(query_part, "tp", axis=1, tiled=True),
        lax.all_gather(latent_part, "tp", axis=1, tiled=True),
    )
    positions = seq_rank * local_rows + jnp.arange(local_rows, dtype=jnp.int32)
    query_normed = latent_norm(query_latent, q_gain)
    key_normed = latent_norm(kv_latent, kv_gain)
    own_heads = w_key.shape[1] // NOPE
    cosine, sine_table = tables(positions, ROPE)
    query_content = (
        jnp.dot(query_normed, w_q_content, preferred_element_type=jnp.float32)
        .astype(jnp.bfloat16)
        .reshape(local_rows, own_heads, NOPE)
    )
    query_rotary = rotate(
        jnp.dot(query_normed, w_q_rotary, preferred_element_type=jnp.float32).reshape(
            local_rows, own_heads, ROPE
        ),
        cosine[:, None, :],
        sine_table[:, None, :],
    ).astype(jnp.bfloat16)
    key_rotary = rotate(rotary_raw.astype(jnp.float32), cosine, sine_table).astype(jnp.bfloat16)
    query = jnp.concatenate(
        [
            query_content,
            query_rotary,
            jnp.zeros((local_rows, own_heads, 2 * NOPE - NOPE - ROPE), jnp.bfloat16),
        ],
        axis=-1,
    ).transpose(1, 0, 2)
    packed = jnp.concatenate(
        [key_normed, key_rotary, jnp.zeros((local_rows, NOPE - ROPE), jnp.bfloat16)], axis=1
    )
    attended, log_rows = attention(seq_count, tp_size, query, packed, w_key, w_value)
    log_total = log_rows[:, : own_heads // 2].reshape(own_heads, local_rows).T
    group_count = pool_cols // GROUP_DIM
    rim_rows = shifted(pool_pre[local_rows - (WIDEST - 1) :], "sp", seq_count)
    rim_rows = jnp.where(seq_rank > 0, rim_rows, jnp.zeros_like(rim_rows))
    pool_values = pool_pre.astype(jnp.float32)
    extended = jnp.concatenate([rim_rows.astype(jnp.float32), pool_values], axis=0)
    groups = tp_rank * group_count + jnp.arange(pool_cols, dtype=jnp.int32) // GROUP_DIM
    windows = jnp.left_shift(jnp.int32(2), groups % 4)
    window_sums = jnp.zeros((local_rows, pool_cols), jnp.float32)
    for distance in range(WIDEST):
        window_sums = window_sums + jnp.where(
            distance < windows[None, :],
            extended[WIDEST - 1 - distance : WIDEST - 1 - distance + local_rows],
            0.0,
        )
    counts = jnp.minimum(positions[:, None] + 1, windows[None, :]).astype(jnp.float32)
    pooled = (window_sums / counts - pool_values).astype(jnp.bfloat16)
    own_mix = lax.dynamic_slice_in_dim(pool_mix, tp_rank * group_count, group_count, 0)
    mixed_pool = jnp.einsum(
        "rgc,gcd->rgd",
        pooled.reshape(local_rows, group_count, GROUP_DIM),
        own_mix,
        preferred_element_type=jnp.float32,
    ).reshape(local_rows, pool_cols)
    own_scale = lax.dynamic_slice_in_dim(pool_scale, tp_rank * pool_cols, pool_cols)
    pool_out = (mixed_pool * own_scale).astype(jnp.bfloat16)
    layer_out = lax.psum_scatter(
        (
            jnp.dot(pool_out, w_out_pool, preferred_element_type=jnp.float32)
            + jnp.dot(attended, w_out_attn, preferred_element_type=jnp.float32)
        ).astype(jnp.bfloat16),
        "tp",
        scatter_dimension=0,
        tiled=True,
    )
    return (layer_out, log_total)


def solution(mesh):
    in_specs = (
        P("sp", "tp"),
        P(),
        P(None, "tp"),
        P(None, "tp"),
        P(None, "tp"),
        P(),
        P(),
        P(),
        P(None, "tp"),
        P(None, "tp"),
        P(None, "tp"),
        P(None, "tp"),
        P(),
        P(),
        P("tp", None),
        P("tp", None),
    )
    out_specs = (P(("sp", "tp"), None), P("sp", "tp"))
    return jax.shard_map(
        per_device, mesh=mesh, in_specs=in_specs, out_specs=out_specs, check_vma=False
    )
```
